32 devices in a mesh: grp: 2 (over y), tp: 4 (over z), dp: 4 (over x, core).
Axes of the slice: x: 2, y: 2, z: 4, core: 2. Of those that a mesh axis runs over, the one named last changes fastest.
Arguments:
- tokens: bfloat16 [128, 2048], P(('grp', 'tp'), 'dp'), parts along dimension 0, may hold values from -200 to 200
- norm_gain: bfloat16 [2, 2048], P(None, 'dp'), may hold values from 0.099609375 to 1.8984375
- w_z: bfloat16 [2, 2048, 4096], P(None, 'dp', 'tp'), may hold values from -0.125 to 0.125
- w_x: bfloat16 [2, 2048, 4096], P(None, 'dp', 'tp'), may hold values from -0.125 to 0.125
- w_b: bfloat16 [2, 2048, 1024], P(None, 'dp', 'tp'), may hold values from -0.125 to 0.125
- w_c: bfloat16 [2, 2048, 1024], P(None, 'dp', 'tp'), may hold values from -0.125 to 0.125
- w_dt: bfloat16 [2, 2048, 64], P(None, 'dp'), may hold values from -0.125 to 0.125
- conv_x: bfloat16 [2, 4, 4096], P(None, None, 'tp'), may hold values from -3 to 3
- conv_b: bfloat16 [2, 4, 1024], P(None, None, 'tp'), may hold values from -3 to 3
- conv_c: bfloat16 [2, 4, 1024], P(None, None, 'tp'), may hold values from -3 to 3
- dt_bias: float32 [2, 64], P(None, 'tp'), may hold values from -3 to 0.5
- a_log: float32 [2, 64], P(None, 'tp'), may hold values from 0 to 2.5
- d_skip: float32 [2, 64], P(None, 'tp'), may hold values from 0.5 to 2
- out_gain: bfloat16 [2, 4096], P(None, 'tp'), may hold values from 0.099609375 to 1.8984375
- w_out: bfloat16 [2, 4096, 2048], P(None, 'tp', 'dp'), may hold values from -0.09375 to 0.09375
- ssm_state: float32 [2, 128, 64, 64, 64], P(None, ('grp', 'dp'), 'tp'), parts along dimension 1, may hold values from -3 to 3
- state_x: bfloat16 [2, 128, 3, 4096], P(None, ('grp', 'dp'), None, 'tp'), parts along dimension 1, may hold values from -6 to 6
- state_b: bfloat16 [2, 128, 3, 1024], P(None, ('grp', 'dp'), None, 'tp'), parts along dimension 1, may hold values from -6 to 6
- state_c: bfloat16 [2, 128, 3, 1024], P(None, ('grp', 'dp'), None, 'tp'), parts along dimension 1, may hold values from -6 to 6
Outputs:
- residual: bfloat16 [128, 2048], P(('grp', 'tp'), 'dp'), parts along dimension 0
- ssm_next: float32 [2, 128, 64, 64, 64], P(None, ('grp', 'dp'), 'tp'), parts along dimension 1
- next_x: bfloat16 [2, 128, 3, 4096], P(None, ('grp', 'dp'), None, 'tp'), parts along dimension 1
- next_b: bfloat16 [2, 128, 3, 1024], P(None, ('grp', 'dp'), None, 'tp'), parts along dimension 1
- next_c: bfloat16 [2, 128, 3, 1024], P(None, ('grp', 'dp'), None, 'tp'), parts along dimension 1
The draws below stay inside these ranges and needn't reach their ends.
There are 2 independent parts, one for each index of `grp`. The reference program is written for one: setup_inputs(seed, part) draws one part's arguments, and reference() takes and returns one part's arrays. A program takes and returns all parts, laid end to end along the dimension named above; an argument that names none is the same for every part. Nothing has to cross between parts.
All inputs are finite; a program needn't handle non-finite values.
Results may differ from the reference program's by a relative error of at most 0.0095.
Values may be sent and summed in bfloat16 or wider, within the bound.
No kernel may reach another device: no remote copies, remote signals or barrier semaphores. Data moves between devices by JAX's collectives and lax.ppermute only.
A program may use at most 128 MiB of HBM per device.

```python
import jax
import jax.numpy as jnp
from jax import lax

D = 2048
HEADS = 64
HEAD_DIM = 64
GROUPS = 16
STATE = 64
KW = 4
LAYERS = 2
SW = 4096
SEQS = 64


def draw_tokens(key, part):
    ramp = jnp.exp(jnp.log(4.0) * jnp.arange(D, dtype=jnp.float32) / D)
    values = jnp.clip(jax.random.normal(jax.random.fold_in(key, 13), (SEQS, D), jnp.float32), -5.0, 5.0)
    return (values * ramp[None, :]).astype(jnp.bfloat16)


def block_levels(key, shape, cuts, low, high):
    level = 1.0
    for axis_at, blocks in cuts:
        steps = jax.random.uniform(jax.random.fold_in(jax.random.fold_in(key, 6), axis_at), (blocks,), jnp.float32, low / len(cuts), high / len(cuts))
        level = level * jnp.repeat(jnp.exp(steps), shape[axis_at] // blocks).reshape((-1,) + (1,) * (len(shape) - 1 - axis_at))
    return level


def normal_values(rng, dims, spread, most, split=(), kind=jnp.bfloat16):
    level = block_levels(rng, dims, split, -0.22, 0.18) if split else 1.0
    drawn = jax.random.normal(rng, dims, jnp.float32) * spread * level
    return jnp.minimum(jnp.maximum(drawn, -most), most).astype(kind)


def setup_inputs(seed: int = 0, part: int = 0) -> dict:
    arg_keys = jax.random.split(jax.random.key(seed), 20)
    part_splits = jax.random.split(jax.random.fold_in(arg_keys[19], part), 20)
    tokens = draw_tokens(jax.random.fold_in(jax.random.fold_in(arg_keys[19], part), 71), part)
    norm_gain = jnp.clip(1.0 + 0.18 * jax.random.normal(arg_keys[1], (LAYERS, D), jnp.float32), 0.099609375, 1.8984375).astype(jnp.bfloat16)
    w_z = normal_values(arg_keys[2], (LAYERS, D, SW), D ** -0.5, 0.125, ((1, 4), (2, 4)))
    w_x = normal_values(arg_keys[3], (LAYERS, D, SW), D ** -0.5, 0.125, ((1, 4), (2, 4)))
    w_b = normal_values(arg_keys[4], (LAYERS, D, GROUPS * STATE), D ** -0.5, 0.125, ((1, 4), (2, 4)))
    w_c = normal_values(arg_keys[5], (LAYERS, D, GROUPS * STATE), D ** -0.5, 0.125, ((1, 4), (2, 4)))
    w_dt = normal_values(arg_keys[6], (LAYERS, D, HEADS), D ** -0.5, 0.125, ((1, 4),))
    conv_x = normal_values(arg_keys[7], (LAYERS, KW, SW), 0.5, 3.0, ((2, 4),))
    conv_b = normal_values(arg_keys[8], (LAYERS, KW, GROUPS * STATE), 0.5, 3.0, ((2, 4),))
    conv_c = normal_values(arg_keys[9], (LAYERS, KW, GROUPS * STATE), 0.5, 3.0, ((2, 4),))
    dt_bias = jnp.clip(-3.0 + 3.5 * jax.random.uniform(arg_keys[10], (LAYERS, HEADS), jnp.float32) ** block_levels(arg_keys[10], (LAYERS, HEADS), ((1, 4),), -0.2, 0.2), -3.0, 0.5)
    a_log = jnp.clip(2.5 * jax.random.uniform(arg_keys[11], (LAYERS, HEADS), jnp.float32) ** block_levels(arg_keys[11], (LAYERS, HEADS), ((1, 4),), -0.2, 0.2), 0.0, 2.5)
    d_skip = jnp.clip(0.5 + 1.5 * jax.random.uniform(arg_keys[12], (LAYERS, HEADS), jnp.float32) ** block_levels(arg_keys[12], (LAYERS, HEADS), ((1, 4),), -0.2, 0.2), 0.5, 2.0)
    out_gain = jnp.clip(1.0 + 0.18 * jax.random.normal(arg_keys[13], (LAYERS, SW), jnp.float32), 0.099609375, 1.8984375).astype(jnp.bfloat16)
    w_out = normal_values(arg_keys[14], (LAYERS, SW, D), SW ** -0.5, 0.09375, ((1, 4), (2, 4)))
    ssm_state = normal_values(part_splits[15], (LAYERS, SEQS, HEADS, HEAD_DIM, STATE), 0.5, 3.0, ((1, 4), (2, 4)), jnp.float32)
    state_x = normal_values(part_splits[16], (LAYERS, SEQS, KW - 1, SW), 1.0, 6.0, ((1, 4), (3, 4)))
    state_b = normal_values(part_splits[17], (LAYERS, SEQS, KW - 1, GROUPS * STATE), 1.0, 6.0, ((1, 4), (3, 4)))
    state_c = normal_values(part_splits[18], (LAYERS, SEQS, KW - 1, GROUPS * STATE), 1.0, 6.0, ((1, 4), (3, 4)))
    return {"tokens": tokens, "norm_gain": norm_gain, "w_z": w_z, "w_x": w_x, "w_b": w_b, "w_c": w_c, "w_dt": w_dt, "conv_x": conv_x, "conv_b": conv_b, "conv_c": conv_c, "dt_bias": dt_bias, "a_log": a_log, "d_skip": d_skip, "out_gain": out_gain, "w_out": w_out, "ssm_state": ssm_state, "state_x": state_x, "state_b": state_b, "state_c": state_c}


EPSILON = 1e-05

def convolve(history, latest, weight):
    window = jnp.concatenate([history, latest[:, None, :]], axis=1)
    summed = lax.optimization_barrier(jnp.sum(window.astype(jnp.float32) * weight.astype(jnp.float32)[None], axis=1))
    return (jax.nn.silu(summed), window[:, 1:])

def mixer(gate_in, conv_xv, conv_bv, conv_cv, step_raw, bias, log_rate, skip, gain, state_prev):
    seq_count = conv_xv.shape[0]
    heads_here = step_raw.shape[1]
    group_count = conv_bv.shape[1] // STATE
    per_group = heads_here // group_count
    step_size = jax.nn.softplus(step_raw + bias)
    decay_rate = jnp.exp(-step_size * jnp.exp(log_rate))
    x_heads = conv_xv.reshape(seq_count, group_count, per_group, HEAD_DIM)
    b_state = conv_bv.reshape(seq_count, group_count, 1, 1, STATE)
    c_state = conv_cv.reshape(seq_count, group_count, 1, 1, STATE)
    step_heads = step_size.reshape(seq_count, group_count, per_group, 1)
    decay_heads = decay_rate.reshape(seq_count, group_count, per_group, 1, 1)
    previous = state_prev.reshape(seq_count, group_count, per_group, HEAD_DIM, STATE)
    state_next = decay_heads * previous + (step_heads * x_heads)[..., None] * b_state
    readout = lax.optimization_barrier(jnp.sum(state_next * c_state, axis=-1)) + skip.reshape(1, group_count, per_group, 1) * x_heads
    gated_out = readout.reshape(seq_count, group_count, -1) * jax.nn.silu(gate_in.astype(jnp.float32)).reshape(seq_count, group_count, -1)
    normed = gated_out * lax.rsqrt(lax.optimization_barrier(jnp.mean(gated_out * gated_out, axis=-1, keepdims=True)) + EPSILON)
    mixed_out = (normed.reshape(seq_count, -1) * gain.astype(jnp.float32)).astype(jnp.bfloat16)
    return (mixed_out, state_next.reshape(seq_count, heads_here, HEAD_DIM, STATE))

def reference(tokens, norm_gain, w_z, w_x, w_b, w_c, w_dt, conv_x, conv_b, conv_c, dt_bias, a_log, d_skip, out_gain, w_out, ssm_state, state_x, state_b, state_c):
    residual = tokens
    states, saved_x, saved_b, saved_c = ([], [], [], [])
    for layer_index in range(LAYERS):
        widened = residual.astype(jnp.float32)
        row_scale = lax.rsqrt(lax.optimization_barrier(jnp.mean(widened * widened, axis=1, keepdims=True)) + EPSILON)
        scaled = (widened * norm_gain[layer_index].astype(jnp.float32)).astype(jnp.bfloat16)
        gate_in = (jnp.dot(scaled, w_z[layer_index], preferred_element_type=jnp.float32) * row_scale).astype(jnp.bfloat16)
        x_in = (jnp.dot(scaled, w_x[layer_index], preferred_element_type=jnp.float32) * row_scale).astype(jnp.bfloat16)
        b_in = (jnp.dot(scaled, w_b[layer_index], preferred_element_type=jnp.float32) * row_scale).astype(jnp.bfloat16)
        c_in = (jnp.dot(scaled, w_c[layer_index], preferred_element_type=jnp.float32) * row_scale).astype(jnp.bfloat16)
        step_raw = jnp.dot(scaled, w_dt[layer_index], preferred_element_type=jnp.float32) * row_scale
        conv_xv, kept_x = convolve(state_x[layer_index], x_in, conv_x[layer_index])
        conv_bv, kept_b = convolve(state_b[layer_index], b_in, conv_b[layer_index])
        conv_cv, kept_c = convolve(state_c[layer_index], c_in, conv_c[layer_index])
        mixed_out, state_next = mixer(gate_in, conv_xv, conv_bv, conv_cv, step_raw, dt_bias[layer_index], a_log[layer_index], d_skip[layer_index], out_gain[layer_index], ssm_state[layer_index])
        projected = jnp.dot(mixed_out, w_out[layer_index], preferred_element_type=jnp.float32)
        residual = (widened + projected).astype(jnp.bfloat16)
        states.append(state_next)
        saved_x.append(kept_x)
        saved_b.append(kept_b)
        saved_c.append(kept_c)
    return (residual, jnp.stack(states), jnp.stack(saved_x), jnp.stack(saved_b), jnp.stack(saved_c))
```

```python
import jax
import jax.numpy as jnp
from jax import lax
from jax.sharding import PartitionSpec as P

HEAD_DIM = 64
STATE = 64


EPSILON = 1e-05


def convolve(history, latest, weight):
    window = jnp.concatenate([history, latest[:, None, :]], axis=1)
    summed = jnp.sum(window.astype(jnp.float32) * weight.astype(jnp.float32)[None], axis=1)
    return (jax.nn.silu(summed), window[:, 1:])


def mixer(gate_in, conv_xv, conv_bv, conv_cv, step_raw, bias, log_rate, skip, gain, state_prev):
    seq_count = conv_xv.shape[0]
    heads_here = step_raw.shape[1]
    group_count = conv_bv.shape[1] // STATE
    per_group = heads_here // group_count
    step_size = jax.nn.softplus(step_raw + bias)
    decay_rate = jnp.exp(-step_size * jnp.exp(log_rate))
    x_heads = conv_xv.reshape(seq_count, group_count, per_group, HEAD_DIM)
    b_state = conv_bv.reshape(seq_count, group_count, 1, 1, STATE)
    c_state = conv_cv.reshape(seq_count, group_count, 1, 1, STATE)
    step_heads = step_size.reshape(seq_count, group_count, per_group, 1)
    decay_heads = decay_rate.reshape(seq_count, group_count, per_group, 1, 1)
    previous = state_prev.reshape(seq_count, group_count, per_group, HEAD_DIM, STATE)
    state_next = decay_heads * previous + (step_heads * x_heads)[..., None] * b_state
    readout = (
        jnp.sum(state_next * c_state, axis=-1)
        + skip.reshape(1, group_count, per_group, 1) * x_heads
    )
    gated_out = readout.reshape(seq_count, group_count, -1) * jax.nn.silu(
        gate_in.astype(jnp.float32)
    ).reshape(seq_count, group_count, -1)
    normed = gated_out * lax.rsqrt(
        jnp.mean(gated_out * gated_out, axis=-1, keepdims=True) + EPSILON
    )
    mixed_out = (normed.reshape(seq_count, -1) * gain.astype(jnp.float32)).astype(jnp.bfloat16)
    return (mixed_out, state_next.reshape(seq_count, heads_here, HEAD_DIM, STATE))


def block_at(stacked, index):
    return lax.dynamic_index_in_dim(stacked, index, 0, keepdims=False)


def shift_gather(value, axis):
    size = lax.axis_size(axis)
    moved = [value]
    for shift in range(1, size):
        moved.append(lax.ppermute(value, axis, [(i, (i + shift) % size) for i in range(size)]))
    return jnp.stack(moved)


def shift_exchange(blocks, axis, wire):
    size = lax.axis_size(axis)
    here = lax.axis_index(axis)
    own = blocks(here)
    received = []
    for shift in range(1, size):
        outgoing = blocks((here + shift) % size).astype(wire)
        received.append(
            lax.ppermute(outgoing, axis, [(i, (i + shift) % size) for i in range(size)])
        )
    return own, received


def split_pair(value):
    high = value.astype(jnp.bfloat16)
    low = (value - high.astype(jnp.float32)).astype(jnp.bfloat16)
    return high, low


def body(
    tokens,
    norm_gain,
    w_z,
    w_x,
    w_b,
    w_c,
    w_dt,
    conv_x,
    conv_b,
    conv_c,
    dt_bias,
    a_log,
    d_skip,
    out_gain,
    w_out,
    ssm_state,
    state_x,
    state_b,
    state_c,
):
    dp_size = lax.axis_size("dp")
    tp_size = lax.axis_size("tp")
    tp_here = lax.axis_index("tp")
    dp_here = lax.axis_index("dp")
    residual = tokens
    states, saved_x, saved_b, saved_c = ([], [], [], [])
    width_z = w_z.shape[2]
    width_b = w_b.shape[2]
    heads_here = dt_bias.shape[1]
    rows = tokens.shape[0]
    features = tokens.shape[1] * dp_size
    for layer_index in range(w_z.shape[0]):
        gathered = shift_gather(residual, "tp")
        widened = gathered.reshape(tp_size * rows, -1).astype(jnp.float32)
        squares = jnp.sum(widened * widened, axis=1, keepdims=True)
        scaled = (widened * norm_gain[layer_index].astype(jnp.float32)).astype(jnp.bfloat16)
        w_step = lax.dynamic_slice_in_dim(w_dt[layer_index], tp_here * heads_here, heads_here, 1)
        mats = (w_z[layer_index], w_x[layer_index], w_b[layer_index], w_c[layer_index])
        main = jnp.concatenate(
            [jnp.dot(scaled, m, preferred_element_type=jnp.float32).astype(jnp.bfloat16) for m in mats], axis=1
        )
        step_part = jnp.dot(scaled, w_step, preferred_element_type=jnp.float32)
        high, low = split_pair(jnp.concatenate([step_part, squares], axis=1))
        merged = jnp.concatenate([main, high, low], axis=1)
        stacked = merged.reshape(tp_size, rows, -1)
        own, received = shift_exchange(
            lambda d: block_at(stacked, (tp_here - d) % tp_size), "dp", jnp.bfloat16)
        total = own.astype(jnp.float32)
        for r in received:
            total = total + r.astype(jnp.float32)
        base = 2 * width_z + 2 * width_b
        tiny = total[:, base : base + heads_here + 1] + total[:, base + heads_here + 1 :]
        row_scale = lax.rsqrt(tiny[:, heads_here:] / features + EPSILON)
        projected_in = (total[:, :base] * row_scale).astype(jnp.bfloat16)
        gate_in = projected_in[:, 0:width_z]
        x_in = projected_in[:, width_z : 2 * width_z]
        b_in = projected_in[:, 2 * width_z : 2 * width_z + width_b]
        c_in = projected_in[:, 2 * width_z + width_b :]
        step_raw = tiny[:, :heads_here] * row_scale
        conv_xv, kept_x = convolve(state_x[layer_index], x_in, conv_x[layer_index])
        conv_bv, kept_b = convolve(state_b[layer_index], b_in, conv_b[layer_index])
        conv_cv, kept_c = convolve(state_c[layer_index], c_in, conv_c[layer_index])
        mixed_out, state_next = mixer(
            gate_in, conv_xv, conv_bv, conv_cv, step_raw, dt_bias[layer_index], a_log[layer_index],
            d_skip[layer_index], out_gain[layer_index], ssm_state[layer_index],
        )
        all_mixed = shift_gather(mixed_out, "dp")
        partial = jnp.dot(
            all_mixed.reshape(dp_size * mixed_out.shape[0], -1), w_out[layer_index], preferred_element_type=jnp.float32
        ).reshape(dp_size, mixed_out.shape[0], -1)
        own, received = shift_exchange(
            lambda t: block_at(partial, (dp_here - t) % dp_size), "tp", jnp.bfloat16)
        projected = own
        for r in received:
            projected = projected + r.astype(jnp.float32)
        residual = (residual.astype(jnp.float32) + projected).astype(jnp.bfloat16)
        states.append(state_next)
        saved_x.append(kept_x)
        saved_b.append(kept_b)
        saved_c.append(kept_c)
    return (residual, jnp.stack(states), jnp.stack(saved_x), jnp.stack(saved_b), jnp.stack(saved_c))


def solution(mesh):
    placed = (
        P(("grp", "tp"), "dp"),
        P(None, "dp"),
        P(None, "dp", "tp"),
        P(None, "dp", "tp"),
        P(None, "dp", "tp"),
        P(None, "dp", "tp"),
        P(None, "dp", None),
        P(None, None, "tp"),
        P(None, None, "tp"),
        P(None, None, "tp"),
        P(None, "tp"),
        P(None, "tp"),
        P(None, "tp"),
        P(None, "tp"),
        P(None, "tp", "dp"),
        P(None, ("grp", "dp"), "tp", None, None),
        P(None, ("grp", "dp"), None, "tp"),
        P(None, ("grp", "dp"), None, "tp"),
        P(None, ("grp", "dp"), None, "tp"),
    )
    return jax.shard_map(
        body,
        mesh=mesh,
        in_specs=placed,
        out_specs=(
            P(("grp", "tp"), "dp"),
            P(None, ("grp", "dp"), "tp", None, None),
            P(None, ("grp", "dp"), None, "tp"),
            P(None, ("grp", "dp"), None, "tp"),
            P(None, ("grp", "dp"), None, "tp"),
        ),
        check_vma=False,
    )
```

```python
import jax
import jax.numpy as jnp
from jax import lax
from jax.experimental import pallas as pl
from jax.sharding import PartitionSpec as P

HEAD_DIM = 64
STATE = 64


EPSILON = 1e-05


def convolve(history, latest, weight):
    window = jnp.concatenate([history, latest[:, None, :]], axis=1)
    summed = jnp.sum(window.astype(jnp.float32) * weight.astype(jnp.float32)[None], axis=1)
    return (jax.nn.silu(summed), window[:, 1:])


def mixer(gate_in, conv_xv, conv_bv, conv_cv, step_raw, bias, log_rate, skip, gain, state_prev):
    seq_count = conv_xv.shape[0]
    heads_here = step_raw.shape[1]
    group_count = conv_bv.shape[1] // STATE
    per_group = heads_here // group_count
    step_size = jax.nn.softplus(step_raw + bias)
    decay_rate = jnp.exp(-step_size * jnp.exp(log_rate))
    x_heads = conv_xv.reshape(seq_count, group_count, per_group, HEAD_DIM)
    b_state = conv_bv.reshape(seq_count, group_count, 1, 1, STATE)
    c_state = conv_cv.reshape(seq_count, group_count, 1, 1, STATE)
    step_heads = step_size.reshape(seq_count, group_count, per_group, 1)
    decay_heads = decay_rate.reshape(seq_count, group_count, per_group, 1, 1)
    previous = state_prev.reshape(seq_count, group_count, per_group, HEAD_DIM, STATE)
    state_next = decay_heads * previous + (step_heads * x_heads)[..., None] * b_state
    readout = (
        jnp.sum(state_next * c_state, axis=-1)
        + skip.reshape(1, group_count, per_group, 1) * x_heads
    )
    gated_out = readout.reshape(seq_count, group_count, -1) * jax.nn.silu(
        gate_in.astype(jnp.float32)
    ).reshape(seq_count, group_count, -1)
    normed = gated_out * lax.rsqrt(
        jnp.mean(gated_out * gated_out, axis=-1, keepdims=True) + EPSILON
    )
    mixed_out = (normed.reshape(seq_count, -1) * gain.astype(jnp.float32)).astype(jnp.bfloat16)
    return (mixed_out, state_next.reshape(seq_count, heads_here, HEAD_DIM, STATE))

def unwritten(like):
    return pl.pallas_call(
        lambda out_ref: None,
        out_shape=jax.ShapeDtypeStruct(like.shape, like.dtype),
        out_specs=pl.BlockSpec(memory_space=pl.ANY),
        name="unwritten",
    )()


def block_at(stacked, index):
    return lax.dynamic_index_in_dim(stacked, index, 0, keepdims=False)


def shift_gather(value, axis):
    size = lax.axis_size(axis)
    moved = [value]
    for shift in range(1, size):
        moved.append(lax.ppermute(value, axis, [(i, (i + shift) % size) for i in range(size)]))
    return jnp.stack(moved)


def shift_exchange(blocks, axis, wire):
    size = lax.axis_size(axis)
    here = lax.axis_index(axis)
    own = blocks(here)
    received = []
    for shift in range(1, size):
        outgoing = blocks((here + shift) % size).astype(wire)
        received.append(
            lax.ppermute(outgoing, axis, [(i, (i + shift) % size) for i in range(size)])
        )
    return own, received


def split_pair(value):
    high = value.astype(jnp.bfloat16)
    low = (value - high.astype(jnp.float32)).astype(jnp.bfloat16)
    return high, low


def body(
    tokens,
    norm_gain,
    w_z,
    w_x,
    w_b,
    w_c,
    w_dt,
    conv_x,
    conv_b,
    conv_c,
    dt_bias,
    a_log,
    d_skip,
    out_gain,
    w_out,
    ssm_state,
    state_x,
    state_b,
    state_c,
):
    dp_size = lax.axis_size("dp")
    tp_size = lax.axis_size("tp")
    tp_here = lax.axis_index("tp")
    dp_here = lax.axis_index("dp")
    residual = tokens
    written = unwritten(ssm_state)
    saved_x, saved_b, saved_c = ([], [], [])
    width_z = w_z.shape[2]
    width_b = w_b.shape[2]
    heads_here = dt_bias.shape[1]
    rows = tokens.shape[0]
    features = tokens.shape[1] * dp_size
    for layer_index in range(w_z.shape[0]):
        if layer_index == 0:
            gathered = shift_gather(residual, "tp")
            gathered = jnp.roll(gathered, dp_here - tp_here, axis=0)
        else:
            gathered, state_x, state_b, state_c, conv_x, conv_b, conv_c, w_dt = (
                lax.optimization_barrier(
                    (gathered, state_x, state_b, state_c, conv_x, conv_b, conv_c, w_dt)
                )
            )
        widened = gathered.reshape(tp_size * rows, -1).astype(jnp.float32)
        squares = jnp.sum(widened * widened, axis=1, keepdims=True)
        scaled = (widened * norm_gain[layer_index].astype(jnp.float32)).astype(jnp.bfloat16)
        w_step = lax.dynamic_slice_in_dim(w_dt[layer_index], tp_here * heads_here, heads_here, 1)
        mats = (w_z[layer_index], w_x[layer_index], w_b[layer_index], w_c[layer_index])
        main = jnp.concatenate(
            [jnp.dot(scaled, m, preferred_element_type=jnp.float32).astype(jnp.bfloat16) for m in mats], axis=1
        )
        step_part = jnp.dot(scaled, w_step, preferred_element_type=jnp.float32)
        high, low = split_pair(jnp.concatenate([step_part, squares], axis=1))
        merged = jnp.concatenate([main, high, low], axis=1)
        stacked = merged.reshape(tp_size, rows, -1)
        own, received = shift_exchange(
            lambda d: block_at(stacked, (dp_here - d) % dp_size), "dp", jnp.bfloat16)
        total = own.astype(jnp.float32)
        for r in received:
            total = total + r.astype(jnp.float32)
        base = 2 * width_z + 2 * width_b
        tiny = total[:, base : base + heads_here + 1] + total[:, base + heads_here + 1 :]
        row_scale = lax.rsqrt(tiny[:, heads_here:] / features + EPSILON)
        projected_in = (total[:, :base] * row_scale).astype(jnp.bfloat16)
        gate_in = projected_in[:, 0:width_z]
        x_in = projected_in[:, width_z : 2 * width_z]
        b_in = projected_in[:, 2 * width_z : 2 * width_z + width_b]
        c_in = projected_in[:, 2 * width_z + width_b :]
        step_raw = tiny[:, :heads_here] * row_scale
        conv_xv, kept_x = convolve(state_x[layer_index], x_in, conv_x[layer_index])
        conv_bv, kept_b = convolve(state_b[layer_index], b_in, conv_b[layer_index])
        conv_cv, kept_c = convolve(state_c[layer_index], c_in, conv_c[layer_index])
        mixed_out, state_next = mixer(
            gate_in, conv_xv, conv_bv, conv_cv, step_raw, dt_bias[layer_index], a_log[layer_index],
            d_skip[layer_index], out_gain[layer_index], ssm_state[layer_index],
        )
        all_mixed = shift_gather(mixed_out, "dp")
        partial = jnp.dot(
            all_mixed.reshape(dp_size * mixed_out.shape[0], -1), w_out[layer_index], preferred_element_type=jnp.float32
        ).reshape(dp_size, mixed_out.shape[0], -1)
        if layer_index + 1 < w_z.shape[0]:
            spread = shift_gather(partial.astype(jnp.bfloat16), "tp").astype(jnp.float32)
            gathered = (gathered.astype(jnp.float32) + jnp.sum(spread, axis=0)).astype(jnp.bfloat16)
        else:
            own_rows = block_at(gathered, (dp_here - tp_here) % dp_size)
            own, received = shift_exchange(
                lambda t: block_at(partial, (dp_here - t) % dp_size), "tp", jnp.bfloat16)
            projected = own
            for r in received:
                projected = projected + r.astype(jnp.float32)
            residual = (own_rows.astype(jnp.float32) + projected).astype(jnp.bfloat16)
        written = lax.dynamic_update_slice_in_dim(written, state_next[None], layer_index, 0)
        saved_x.append(kept_x)
        saved_b.append(kept_b)
        saved_c.append(kept_c)
    return (residual, written, jnp.stack(saved_x), jnp.stack(saved_b), jnp.stack(saved_c))


def solution(mesh):
    placed = (
        P(("grp", "tp"), "dp"),
        P(None, "dp"),
        P(None, "dp", "tp"),
        P(None, "dp", "tp"),
        P(None, "dp", "tp"),
        P(None, "dp", "tp"),
        P(None, "dp", None),
        P(None, None, "tp"),
        P(None, None, "tp"),
        P(None, None, "tp"),
        P(None, "tp"),
        P(None, "tp"),
        P(None, "tp"),
        P(None, "tp"),
        P(None, "tp", "dp"),
        P(None, ("grp", "dp"), "tp", None, None),
        P(None, ("grp", "dp"), None, "tp"),
        P(None, ("grp", "dp"), None, "tp"),
        P(None, ("grp", "dp"), None, "tp"),
    )
    return jax.shard_map(
        body,
        mesh=mesh,
        in_specs=placed,
        out_specs=(
            P(("grp", "tp"), "dp"),
            P(None, ("grp", "dp"), "tp", None, None),
            P(None, ("grp", "dp"), None, "tp"),
            P(None, ("grp", "dp"), None, "tp"),
            P(None, ("grp", "dp"), None, "tp"),
        ),
        check_vma=False,
    )
```
